32 devices in a mesh: ep: 8 (over z, x), tp: 4 (over y, core).
Axes of the slice: x: 2, y: 2, z: 4, core: 2. Of those that a mesh axis runs over, the one named last changes fastest.
Arguments:
- tokens: bfloat16 [8192, 2048], P(('ep', 'tp')), may hold values from -6 to 6
- pre_gain: float32 [2048], replicated, may hold values from 0.1 to 1.9
- post_gain: float32 [2048], replicated, may hold values from 0.1 to 1.9
- expert_ids: int32 [8192, 2], P(('ep', 'tp')), may hold values from 0 to 7, as said below
- route_weight: float32 [8192, 2], P(('ep', 'tp')), may hold values from 0.1 to 1
- w_gate: bfloat16 [8, 2048, 512], P('ep', None, 'tp'), may hold values from -0.125 to 0.125
- w_up: bfloat16 [8, 2048, 512], P('ep', None, 'tp'), may hold values from -0.125 to 0.125
- w_down: bfloat16 [8, 2048, 512], P('ep', None, 'tp'), may hold values from -0.25 to 0.25
Outputs:
- layer_out: bfloat16 [8192, 2048], P(('ep', 'tp'))
The draws below stay inside these ranges and needn't reach their ends.
Inputs may be any that keep to these rules, and one draw needn't show every extreme that they name: `expert_ids`: each token names two different experts of one group, group g being experts 4 * g to 4 * g + 3. Among the rows of one device (aligned blocks of 256 rows) no expert is named more than 128 times, and in every block some expert is named exactly 128 times; one expert is named 128 times in every block.
All inputs are finite; a program needn't handle non-finite values.
Results may differ from the reference program's by a relative error of at most 0.0071.
Values may be sent and summed in bfloat16 or wider, within the bound.
A program may use at most 64 MiB of HBM per device.

```python
import math
import jax
import jax.numpy as jnp
from jax import lax

D = 2048
FF = 512
TOP = 2
GROUP = 4
TOK_DEV = 256
EXPERTS = 8
CAP = 128
TOKENS = 8192


def draw_expert_ids(key, part):
    blocks = TOKENS // TOK_DEV
    share = TOP * TOK_DEV // EXPERTS
    pairs = EXPERTS // (2 * GROUP)
    star = jax.random.randint(jax.random.fold_in(key, 11), (), 0, EXPERTS)
    star_group = star // GROUP
    star_pair = star_group // 2
    star_side = star_group % 2
    star_local = star % GROUP
    place = jnp.arange(2 * share * 2, dtype=jnp.int32)
    hot_three = 3 * share
    first_role = jnp.where(place < 2 * share, 0, jnp.where(place < hot_three, 1, jnp.where(place < hot_three + share // 2, 0, 2)))
    second_role = jnp.where(place < share, 1, jnp.where(place < 2 * share, 2, jnp.where(place < hot_three, 3, jnp.where(place < hot_three + share // 2, 1, 3))))
    is_hot = place < hot_three

    def one_block(block):
        block_key = jax.random.fold_in(key, block)
        hot_side = jax.random.randint(jax.random.fold_in(block_key, 1), (pairs,), 0, 2)
        hot_side = jnp.where(jnp.arange(pairs) == star_pair, star_side, hot_side)
        perm_keys = jax.random.split(jax.random.fold_in(block_key, 2), 2 * pairs)
        perms = jax.vmap(lambda sub: jax.random.permutation(sub, GROUP))(perm_keys).astype(jnp.int32)
        star_row = perms[star_group]
        where_star = jnp.argmax(star_row == star_local)
        star_row = star_row.at[where_star].set(star_row[0]).at[0].set(star_local)
        perms = perms.at[star_group].set(star_row)
        pair_index = jnp.arange(pairs, dtype=jnp.int32)[:, None]
        group = 2 * pair_index + jnp.where(is_hot[None, :], hot_side[:, None], 1 - hot_side[:, None])
        first = group * GROUP + perms[group, first_role[None, :]]
        second = group * GROUP + perms[group, second_role[None, :]]
        both = jnp.stack([first.reshape(-1), second.reshape(-1)], axis=1)
        shuffle = jax.random.permutation(jax.random.fold_in(block_key, 3), TOK_DEV)
        return both[shuffle]
    table = lax.map(one_block, jnp.arange(blocks, dtype=jnp.int32))
    return table.reshape(TOKENS, TOP).astype(jnp.int32)


def block_scale(rng, shape, shards, least, high):
    def one(dim, blocks):
        draws = jax.random.uniform(jax.random.fold_in(jax.random.fold_in(rng, 6), dim), (blocks,), jnp.float32, least / len(shards), high / len(shards))
        return jnp.repeat(jnp.exp(draws), shape[dim] // blocks).reshape((-1,) + (1,) * (len(shape) - dim - 1))

    level = one(*shards[0])
    for cut in shards[1:]:
        level = level * one(*cut)
    return level


def bell_draw(key, shape, spread, reach, cuts=(), kind=jnp.bfloat16):
    array = spread * jax.random.normal(key, shape, jnp.float32)
    if cuts:
        array = array * block_scale(key, shape, cuts, -0.22, 0.18)
    return jnp.clip(array, -reach, reach).astype(kind)


def setup_inputs(seed: int = 0) -> dict:
    streams_of = jax.random.split(jax.random.key(seed), 9)
    tokens = bell_draw(streams_of[0], (TOKENS, D), 1.0, 6.0, ((0, 32),))
    pre_gain = jnp.clip(1.0 + 0.18 * jax.random.normal(streams_of[1], (D,), jnp.float32), 0.1, 1.9)
    post_gain = jnp.clip(1.0 + 0.18 * jax.random.normal(streams_of[2], (D,), jnp.float32), 0.1, 1.9)
    expert_ids = draw_expert_ids(jax.random.fold_in(streams_of[8], 71), 0)
    route_weight = jnp.clip(jnp.exp(math.log(1.0) - 2.3025851 * jax.random.uniform(streams_of[4], (TOKENS, TOP), jnp.float32) ** block_scale(streams_of[4], (TOKENS, TOP), ((0, 32),), -0.2, 0.2)), 0.1, 1.0)
    w_gate = bell_draw(streams_of[5], (EXPERTS, D, FF), D ** -0.5, 0.125, ((0, 8), (2, 4)))
    w_up = bell_draw(streams_of[6], (EXPERTS, D, FF), D ** -0.5, 0.125, ((0, 8), (2, 4)))
    w_down = bell_draw(streams_of[7], (EXPERTS, D, FF), FF ** -0.5, 0.25, ((0, 8), (2, 4)))
    return dict(tokens=tokens, pre_gain=pre_gain, post_gain=post_gain, expert_ids=expert_ids, route_weight=route_weight, w_gate=w_gate, w_up=w_up, w_down=w_down)


def rms_scale(values, gain):
    mean_sq = lax.optimization_barrier(jnp.mean(values * values, axis=-1, keepdims=True))
    return values * lax.rsqrt(mean_sq + 1e-06) * gain

def reference(tokens, pre_gain, post_gain, expert_ids, route_weight, w_gate, w_up, w_down):
    count = tokens.shape[0]
    width = tokens.shape[1]
    normed = rms_scale(tokens.astype(jnp.float32), pre_gain).astype(jnp.bfloat16)
    padded = jnp.concatenate([normed, jnp.zeros((1, width), jnp.bfloat16)], axis=0)
    flat = expert_ids.reshape(-1).astype(jnp.int32)
    routes = flat.shape[0]
    order = jnp.argsort(flat, stable=True).astype(jnp.int32)
    sorted_ids = flat[order]
    first = jnp.searchsorted(sorted_ids, sorted_ids, side='left').astype(jnp.int32)
    rank = jnp.arange(routes, dtype=jnp.int32) - first
    global_cap = count // TOK_DEV * CAP
    table = jnp.full((EXPERTS * global_cap,), routes, jnp.int32)
    table = table.at[sorted_ids * global_cap + rank].set(order).reshape(EXPERTS, global_cap)

    def one_expert(index):
        slots = table[index]
        rows = padded[jnp.minimum(slots // TOP, count).astype(jnp.int32)]
        rows = jnp.where((slots < routes)[:, None], rows, jnp.zeros_like(rows))
        gate = jnp.dot(rows, w_gate[index], preferred_element_type=jnp.float32)
        up = jnp.dot(rows, w_up[index], preferred_element_type=jnp.float32)
        hidden = (jax.nn.silu(gate) * up).astype(jnp.bfloat16)
        return jnp.dot(hidden, w_down[index].T, preferred_element_type=jnp.float32).astype(jnp.bfloat16)
    results = lax.map(one_expert, jnp.arange(EXPERTS, dtype=jnp.int32))
    per_route = jnp.zeros((routes + 1, width), jnp.bfloat16)
    per_route = per_route.at[table.reshape(-1)].set(results.reshape(-1, width))
    per_route = per_route[:routes].reshape(count, TOP, width)
    mixed = lax.optimization_barrier(jnp.sum(per_route.astype(jnp.float32) * route_weight[:, :, None], axis=1))
    return rms_scale(mixed, post_gain).astype(jnp.bfloat16)
```

```python
import functools

import jax
import jax.numpy as jnp
from jax import lax
from jax.experimental import pallas as pl
from jax.experimental.pallas import tpu as pltpu
from jax.sharding import PartitionSpec as P


def rms_scale(values, gain):
    mean_sq = jnp.mean(values * values, axis=-1, keepdims=True)
    return values * lax.rsqrt(mean_sq + 1e-06) * gain


def expert_terms(rows, gate_part, up_part, down_part):
    gate = jnp.dot(rows, gate_part, preferred_element_type=jnp.float32)
    up = jnp.dot(rows, up_part, preferred_element_type=jnp.float32)
    hidden = (jax.nn.silu(gate) * up).astype(jnp.bfloat16)
    return lax.dot_general(
        hidden, down_part, (((1,), (1,)), ((), ())), preferred_element_type=jnp.float32
    )


def collect_expert(w_gate, w_up, w_down):
    return (
        lax.all_gather(w_gate, "tp", axis=2, tiled=True),
        lax.all_gather(w_up, "tp", axis=2, tiled=True),
        lax.all_gather(w_down, "tp", axis=2, tiled=True),
    )


def body(tokens, pre_gain, post_gain, expert_ids, route_weight, w_gate, w_up, w_down):
    count, width = tokens.shape
    top = expert_ids.shape[1]
    experts = lax.axis_size("ep") * w_gate.shape[0]
    capacity = 2 * top * count // experts
    normed = rms_scale(tokens.astype(jnp.float32), pre_gain).astype(jnp.bfloat16)
    flat = expert_ids.reshape(-1)
    onehot = (flat[:, None] == jnp.arange(experts, dtype=jnp.int32)[None, :]).astype(jnp.int32)
    rank = jnp.sum((jnp.cumsum(onehot, axis=0) - onehot) * onehot, axis=1)
    target = flat * capacity + rank
    source = jnp.full((experts * capacity,), count, jnp.int32)
    source = source.at[target].set(jnp.arange(count * top, dtype=jnp.int32) // top)
    padded = jnp.concatenate([normed, jnp.zeros((1, width), jnp.bfloat16)], axis=0)
    outgoing = padded[source].reshape(experts, capacity, width)
    arrived = lax.all_to_all(outgoing, "ep", split_axis=0, concat_axis=0, tiled=True)
    rows = arrived.reshape(experts * capacity, width)
    gate_all, up_all, down_all = collect_expert(w_gate, w_up, w_down)
    result = expert_terms(rows, gate_all[0], up_all[0], down_all[0])
    answer = result.astype(jnp.bfloat16).reshape(experts, capacity, width)
    returned = lax.all_to_all(answer, "ep", split_axis=0, concat_axis=0, tiled=True)
    per_route = returned.reshape(experts * capacity, width)[target].reshape(count, top, width)
    mixed = jnp.sum(per_route.astype(jnp.float32) * route_weight[:, :, None], axis=1)
    return rms_scale(mixed, post_gain).astype(jnp.bfloat16)

MESH = pl.DeviceIdType.MESH
GU_CUTS = 2
DOWN_CUTS = 4
VMEM_BYTES = 60 * 2**20


def flip(index, stride):
    return index + stride - 2 * stride * lax.rem(lax.div(index, stride), 2)


def kernel(
    n_ep, tok, pre, post, wr, wg, wu, wd, out,
    T, X, WR, COL, GU, DN, H, S, R, PZ, ZS, ZR, ACC,
    loc, t_send, t_recv, w_send, w_recv, g_send, g_recv, d_send, d_recv, x_send, x_recv, z_send, z_recv,
):
    count, width = tok.shape
    part = wg.shape[2]
    experts = wr.shape[0]
    half = n_ep // 2
    e, t = lax.axis_index("ep"), lax.axis_index("tp")
    to_x, to_z, to_h = (flip(e, 1), t), (flip(e, 2), t), (flip(e, half), t)
    to_c, to_y = (e, flip(t, 1)), (e, flip(t, 2))

    barrier = pltpu.get_barrier_semaphore()
    for who in (to_x, to_z, to_h, to_c, to_y):
        pl.semaphore_signal(barrier, inc=1, device_id=who, device_id_type=MESH)

    own = [
        pltpu.make_async_copy(tok, T.at[0], loc.at[0]),
        pltpu.make_async_copy(wr, WR.at[0], loc.at[1]),
        pltpu.make_async_copy(wg.at[0], GU.at[0, :, pl.ds(0, part)], loc.at[2]),
        pltpu.make_async_copy(wu.at[0], GU.at[0, :, pl.ds(part, part)], loc.at[3]),
        pltpu.make_async_copy(wd.at[0], DN.at[:, pl.ds(0, part)], loc.at[4]),
    ]
    for copy in own:
        copy.start()

    def remote(src, dst, send, recv, who):
        return pltpu.make_async_remote_copy(
            src_ref=src, dst_ref=dst, send_sem=send, recv_sem=recv, device_id=who, device_id_type=MESH
        )

    block_from = {1: (0, to_z), 2: (0, to_x), 3: (1, to_x)}
    sent = []

    def tokens_copy(k):
        s, who = block_from[k]
        return (
            remote(WR.at[s], WR.at[k], w_send.at[k], w_recv.at[k], who),
            remote(T.at[s], T.at[k], t_send.at[k], t_recv.at[k], who),
        )

    def route(k):
        if k % 2:
            return k - 1, to_c
        if k % 4:
            return k - 2, to_y
        return 0, to_h

    g_rows, d_rows = width // GU_CUTS, width // DOWN_CUTS

    def gu_copy(k, j):
        s, who = route(k)
        rows = pl.ds(j * g_rows, g_rows)
        return (remote(GU.at[s, rows], GU.at[k, rows], g_send.at[k, j], g_recv.at[k, j], who),)

    def dn_copy(k, j):
        s, who = route(k)
        rows = pl.ds(j * d_rows, d_rows)
        return (
            remote(
                DN.at[rows, pl.ds(s * part, part)], DN.at[rows, pl.ds(k * part, part)],
                d_send.at[k, j], d_recv.at[k, j], who,
            ),
        )

    def go(copies):
        for copy in copies:
            copy.start()
            sent.append(copy)

    def arrive(copies):
        for copy in copies:
            copy.wait_recv()

    def norm(block):
        rows = pl.ds(block * count, count)

        def some(i, carry):
            part_rows = pl.ds(pl.multiple_of(i * 32, 32), 32)
            values = T[block, part_rows, :].astype(jnp.float32)
            X[block, part_rows, :] = rms_scale(values, pre[...]).astype(jnp.bfloat16)
            return carry

        lax.fori_loop(0, count // 32, some, 0)
        eye = lax.broadcasted_iota(jnp.int32, (count, count), 0) == lax.broadcasted_iota(
            jnp.int32, (count, count), 1
        )
        which = lax.broadcasted_iota(jnp.int32, (experts, count), 0)
        table = WR[block]
        for h in range(2):
            expert = lax.rem(e + h * half, n_ep)
            row = jnp.sum(jnp.where(which == expert, table, 0.0), axis=0, keepdims=True)
            col = jnp.sum(jnp.where(eye, row, 0.0), axis=1, keepdims=True)
            COL[h, rows, :] = jnp.broadcast_to(col, (count, part))

    def hidden(slots, blocks):
        low, high = slots
        first, last = blocks
        span = last - first

        def one(i, carry):
            s = low + lax.div(i, span)
            b = first + lax.rem(i, span)
            rows = pl.ds(pl.multiple_of(b * count, count), count)
            both = jnp.dot(X[b], GU[s], preferred_element_type=jnp.float32)
            gate, up = both[:, :part], both[:, part:]
            value = gate / (1.0 + jnp.exp(-gate)) * up * COL[lax.div(s, 4), rows, :]
            H[rows, pl.ds(pl.multiple_of(s * part, part), part)] = value.astype(jnp.bfloat16)
            return carry

        lax.fori_loop(0, (high - low) * span, one, 0)

    for copy in own[:2]:
        copy.wait()
    pl.semaphore_wait(barrier, 5)
    go(tokens_copy(1))
    go(tokens_copy(2))
    for copy in own[2:4]:
        copy.wait()
    for j in range(GU_CUTS):
        for k in (4, 2, 1):
            go(gu_copy(k, j))
    own[4].wait()
    for j in range(DOWN_CUTS):
        for k in (4, 2, 1):
            go(dn_copy(k, j))
    norm(0)
    for j in range(GU_CUTS):
        arrive(gu_copy(1, j))
    hidden((0, 2), (0, 1))
    arrive(tokens_copy(1))
    go(tokens_copy(3))
    norm(1)
    for j in range(GU_CUTS):
        arrive(gu_copy(2, j))
        go(gu_copy(3, j))
    arrive(tokens_copy(2))
    norm(2)
    hidden((0, 2), (1, 3))
    for j in range(GU_CUTS):
        arrive(gu_copy(4, j))
        go(gu_copy(6, j))
        go(gu_copy(5, j))
    for j in range(GU_CUTS):
        arrive(gu_copy(3, j))
    hidden((2, 4), (0, 3))
    for j in range(DOWN_CUTS):
        arrive(dn_copy(2, j))
        go(dn_copy(3, j))
    for j in range(GU_CUTS):
        arrive(gu_copy(5, j))
    hidden((4, 6), (0, 3))
    arrive(tokens_copy(3))
    norm(3)
    hidden((0, 6), (3, 4))
    for j in range(GU_CUTS):
        arrive(gu_copy(6, j))
        go(gu_copy(7, j))
    arrive(dn_copy(4, 0))
    go(dn_copy(6, 0))
    go(dn_copy(5, 0))
    hidden((6, 7), (0, 4))
    for j in range(GU_CUTS):
        arrive(gu_copy(7, j))
    hidden((7, 8), (0, 4))

    def down(block, j):
        return lax.dot_general(
            H[pl.ds(block * count, count), :], DN[pl.ds(j * d_rows, d_rows), :],
            (((1,), (1,)), ((), ())), preferred_element_type=jnp.float32,
        )

    def x_copy(j):
        return (remote(S.at[j], R.at[j], x_send.at[j], x_recv.at[j], to_x),)

    def z_copy(j):
        return (remote(ZS.at[j], ZR.at[j], z_send.at[j], z_recv.at[j], to_z),)

    def pass_on(j):
        arrive(x_copy(j))
        ZS[j] = (PZ[j] + R[j, count:].astype(jnp.float32)).astype(jnp.bfloat16)
        go(z_copy(j))
        ACC[j] = ACC[j] + R[j, :count].astype(jnp.float32)

    for j in range(DOWN_CUTS):
        arrive(dn_copy(6, j))
        go(dn_copy(7, j))
        if j + 1 < DOWN_CUTS:
            arrive(dn_copy(4, j + 1))
            go(dn_copy(6, j + 1))
            go(dn_copy(5, j + 1))
        for k in (1, 3, 5, 7):
            arrive(dn_copy(k, j))
        S[j, count:] = down(3, j).astype(jnp.bfloat16)
        S[j, :count] = down(2, j).astype(jnp.bfloat16)
        go(x_copy(j))
        PZ[j] = down(1, j)
        ACC[j] = down(0, j)
        if j:
            pass_on(j - 1)
    pass_on(DOWN_CUTS - 1)
    square = jnp.zeros((count, 1), jnp.float32)
    for j in range(DOWN_CUTS):
        arrive(z_copy(j))
        mixed = ACC[j] + ZR[j].astype(jnp.float32)
        ACC[j] = mixed
        square = square + jnp.sum(mixed * mixed, axis=1, keepdims=True)
    scale = lax.rsqrt(square / width + 1e-06)
    for j in range(DOWN_CUTS):
        cols = pl.ds(j * d_rows, d_rows)
        out[:, cols] = (ACC[j] * scale * post[:, cols]).astype(jnp.bfloat16)
    for copy in sent:
        copy.wait_send()


def fused(n_ep, tokens, pre_gain, post_gain, expert_ids, route_weight, w_gate, w_up, w_down):
    count, width = tokens.shape
    part = w_gate.shape[2]
    experts = n_ep * w_gate.shape[0]
    names = jnp.arange(experts, dtype=jnp.int32)[:, None, None]
    picks = jnp.where(expert_ids.T[None] == names, route_weight.T[None], 0.0)
    wr = jnp.sum(picks, axis=1)
    bf, f32 = jnp.bfloat16, jnp.float32
    cols = width // DOWN_CUTS
    anywhere = pl.BlockSpec(memory_space=pl.ANY)
    vmem = pl.BlockSpec(memory_space=pltpu.VMEM)
    dma = pltpu.SemaphoreType.DMA
    return pl.pallas_call(
        functools.partial(kernel, n_ep),
        out_shape=jax.ShapeDtypeStruct((count, width), bf),
        in_specs=[anywhere, vmem, vmem, anywhere, anywhere, anywhere, anywhere],
        out_specs=vmem,
        scratch_shapes=[
            pltpu.VMEM((4, count, width), bf),
            pltpu.VMEM((4, count, width), bf),
            pltpu.VMEM((4, experts, count), f32),
            pltpu.VMEM((2, 4 * count, part), f32),
            pltpu.VMEM((8, width, 2 * part), bf),
            pltpu.VMEM((width, 8 * part), bf),
            pltpu.VMEM((4 * count, 8 * part), bf),
            pltpu.VMEM((DOWN_CUTS, 2 * count, cols), bf),
            pltpu.VMEM((DOWN_CUTS, 2 * count, cols), bf),
            pltpu.VMEM((DOWN_CUTS, count, cols), f32),
            pltpu.VMEM((DOWN_CUTS, count, cols), bf),
            pltpu.VMEM((DOWN_CUTS, count, cols), bf),
            pltpu.VMEM((DOWN_CUTS, count, cols), f32),
            dma((5,)),
            dma((4,)), dma((4,)), dma((4,)), dma((4,)),
            dma((8, GU_CUTS)), dma((8, GU_CUTS)), dma((8, DOWN_CUTS)), dma((8, DOWN_CUTS)),
            dma((DOWN_CUTS,)), dma((DOWN_CUTS,)), dma((DOWN_CUTS,)), dma((DOWN_CUTS,)),
        ],
        compiler_params=pltpu.CompilerParams(
            collective_id=0, has_side_effects=True, vmem_limit_bytes=VMEM_BYTES
        ),
    )(tokens, pre_gain[None], post_gain[None], wr, w_gate, w_up, w_down)


def whole_body(n_ep, n_tp, *args):
    lanes = args[5].shape[2]
    if n_ep // 2 == n_tp == 2 * 2 and args[5].shape[0] == 1 and lanes % 128 == 0:
        return fused(n_ep, *args)
    return body(*args)


def solution(mesh):
    in_specs = (
        P(("ep", "tp"), None),
        P(),
        P(),
        P(("ep", "tp"), None),
        P(("ep", "tp"), None),
        P("ep", None, "tp"),
        P("ep", None, "tp"),
        P("ep", None, "tp"),
    )
    out_specs = P(("ep", "tp"), None)
    step = functools.partial(whole_body, mesh.shape["ep"], mesh.shape["tp"])
    return jax.shard_map(step, mesh=mesh, in_specs=in_specs, out_specs=out_specs, check_vma=False)
```

```python
import functools

import jax
import jax.numpy as jnp
from jax import lax
from jax.experimental import pallas as pl
from jax.experimental.pallas import tpu as pltpu
from jax.sharding import PartitionSpec as P


def rms_scale(values, gain):
    mean_sq = jnp.mean(values * values, axis=-1, keepdims=True)
    return values * lax.rsqrt(mean_sq + 1e-06) * gain


def expert_terms(rows, gate_part, up_part, down_part):
    gate = jnp.dot(rows, gate_part, preferred_element_type=jnp.float32)
    up = jnp.dot(rows, up_part, preferred_element_type=jnp.float32)
    hidden = (jax.nn.silu(gate) * up).astype(jnp.bfloat16)
    return lax.dot_general(
        hidden, down_part, (((1,), (1,)), ((), ())), preferred_element_type=jnp.float32
    )


def collect_expert(w_gate, w_up, w_down):
    return (
        lax.all_gather(w_gate, "tp", axis=2, tiled=True),
        lax.all_gather(w_up, "tp", axis=2, tiled=True),
        lax.all_gather(w_down, "tp", axis=2, tiled=True),
    )


def body(tokens, pre_gain, post_gain, expert_ids, route_weight, w_gate, w_up, w_down):
    count, width = tokens.shape
    top = expert_ids.shape[1]
    experts = lax.axis_size("ep") * w_gate.shape[0]
    capacity = 2 * top * count // experts
    normed = rms_scale(tokens.astype(jnp.float32), pre_gain).astype(jnp.bfloat16)
    flat = expert_ids.reshape(-1)
    onehot = (flat[:, None] == jnp.arange(experts, dtype=jnp.int32)[None, :]).astype(jnp.int32)
    rank = jnp.sum((jnp.cumsum(onehot, axis=0) - onehot) * onehot, axis=1)
    target = flat * capacity + rank
    source = jnp.full((experts * capacity,), count, jnp.int32)
    source = source.at[target].set(jnp.arange(count * top, dtype=jnp.int32) // top)
    padded = jnp.concatenate([normed, jnp.zeros((1, width), jnp.bfloat16)], axis=0)
    outgoing = padded[source].reshape(experts, capacity, width)
    arrived = lax.all_to_all(outgoing, "ep", split_axis=0, concat_axis=0, tiled=True)
    rows = arrived.reshape(experts * capacity, width)
    gate_all, up_all, down_all = collect_expert(w_gate, w_up, w_down)
    result = expert_terms(rows, gate_all[0], up_all[0], down_all[0])
    answer = result.astype(jnp.bfloat16).reshape(experts, capacity, width)
    returned = lax.all_to_all(answer, "ep", split_axis=0, concat_axis=0, tiled=True)
    per_route = returned.reshape(experts * capacity, width)[target].reshape(count, top, width)
    mixed = jnp.sum(per_route.astype(jnp.float32) * route_weight[:, :, None], axis=1)
    return rms_scale(mixed, post_gain).astype(jnp.bfloat16)

MESH = pl.DeviceIdType.MESH
GU_CUTS = 8
DOWN_CUTS = 8
LAG = 5
TOKEN_CUTS = 8
VMEM_BYTES = 60 * 2**20


def flip(index, stride):
    return index + stride - 2 * stride * lax.rem(lax.div(index, stride), 2)


def kernel(
    n_ep, tok, pre, post, wr, wg, wu, wd, out,
    T, X, WR, COL, GU, DN, H, S, R, PZ, ZS, ZR, ACC,
    loc, t_send, t_recv, w_send, w_recv, g_send, g_recv, d_send, d_recv, x_send, x_recv, z_send, z_recv,
):
    count, width = tok.shape
    part = wg.shape[2]
    experts = wr.shape[0]
    half = n_ep // 2
    e, t = lax.axis_index("ep"), lax.axis_index("tp")
    to_x, to_z, to_h = (flip(e, 1), t), (flip(e, 2), t), (flip(e, half), t)
    to_c, to_y = (e, flip(t, 1)), (e, flip(t, 2))

    barrier = pltpu.get_barrier_semaphore()
    for who in (to_x, to_z, to_h, to_c, to_y):
        pl.semaphore_signal(barrier, inc=1, device_id=who, device_id_type=MESH)

    own = [
        pltpu.make_async_copy(tok, T.at[0], loc.at[0]),
        pltpu.make_async_copy(wr, WR.at[0], loc.at[1]),
        pltpu.make_async_copy(wg.at[0], GU.at[0, :, pl.ds(0, part)], loc.at[2]),
        pltpu.make_async_copy(wu.at[0], GU.at[0, :, pl.ds(part, part)], loc.at[3]),
        pltpu.make_async_copy(wd.at[0], DN.at[:, pl.ds(0, part)], loc.at[4]),
    ]
    for copy in own:
        copy.start()

    def remote(src, dst, send, recv, who):
        return pltpu.make_async_remote_copy(
            src_ref=src, dst_ref=dst, send_sem=send, recv_sem=recv, device_id=who, device_id_type=MESH
        )

    block_from = {1: (0, to_z), 2: (0, to_x), 3: (1, to_x)}
    sent = []

    def routes_copy(k):
        s, who = block_from[k]
        return (remote(WR.at[s], WR.at[k], w_send.at[k], w_recv.at[k], who),)

    t_rows = count // TOKEN_CUTS

    def tokens_copy(k, j):
        s, who = block_from[k]
        rows = pl.ds(j * t_rows, t_rows)
        return (remote(T.at[s, rows], T.at[k, rows], t_send.at[k, j], t_recv.at[k, j], who),)

    def route(k):
        if k % 2:
            return k - 1, to_c
        if k % 4:
            return k - 2, to_y
        return 0, to_h

    g_rows, d_rows = width // GU_CUTS, width // DOWN_CUTS

    def gu_copy(k, j):
        s, who = route(k)
        rows = pl.ds(j * g_rows, g_rows)
        return (remote(GU.at[s, rows], GU.at[k, rows], g_send.at[k, j], g_recv.at[k, j], who),)

    def dn_copy(k, j):
        s, who = route(k)
        rows = pl.ds(j * d_rows, d_rows)
        return (
            remote(
                DN.at[rows, pl.ds(s * part, part)], DN.at[rows, pl.ds(k * part, part)],
                d_send.at[k, j], d_recv.at[k, j], who,
            ),
        )

    def go(copies):
        for copy in copies:
            copy.start()
            sent.append(copy)

    def arrive(copies):
        for copy in copies:
            copy.wait_recv()

    def norm(block):
        rows = pl.ds(block * count, count)

        def some(i, carry):
            part_rows = pl.ds(pl.multiple_of(i * 32, 32), 32)
            values = T[block, part_rows, :].astype(jnp.float32)
            X[pl.ds(pl.multiple_of(block * count + i * 32, 32), 32), :] = rms_scale(values, pre[...]).astype(jnp.bfloat16)
            return carry

        lax.fori_loop(0, count // 32, some, 0)
        eye = lax.broadcasted_iota(jnp.int32, (count, count), 0) == lax.broadcasted_iota(
            jnp.int32, (count, count), 1
        )
        which = lax.broadcasted_iota(jnp.int32, (experts, count), 0)
        table = WR[block]
        for h in range(2):
            expert = lax.rem(e + h * half, n_ep)
            row = jnp.sum(jnp.where(which == expert, table, 0.0), axis=0, keepdims=True)
            col = jnp.sum(jnp.where(eye, row, 0.0), axis=1, keepdims=True)
            COL[h, rows, :] = jnp.broadcast_to(col, (count, part))

    def hidden(slots, blocks):
        low, high = slots
        first, last = blocks
        rows = pl.ds(first * count, (last - first) * count)

        def one(s, carry):
            left = X[rows, :]
            both = jnp.dot(left, GU[s], preferred_element_type=jnp.float32)
            gate, up = both[:, :part], both[:, part:]
            value = gate / (1.0 + jnp.exp(-gate)) * up * COL[lax.div(s, 4), rows, :]
            H[rows, pl.ds(pl.multiple_of(s * part, part), part)] = value.astype(jnp.bfloat16)
            return carry

        lax.fori_loop(low, high, one, 0)

    for copy in own[:2]:
        copy.wait()
    pl.semaphore_wait(barrier, 5)
    for k in (1, 2):
        go(routes_copy(k))
    for copy in own[2:4]:
        copy.wait()
    for j in range(TOKEN_CUTS):
        go(tokens_copy(1, j))
        go(tokens_copy(2, j))
        for i in range(j * GU_CUTS // TOKEN_CUTS, (j + 1) * GU_CUTS // TOKEN_CUTS):
            for k in (4, 2, 1):
                go(gu_copy(k, i))
    own[4].wait()
    for j in range(DOWN_CUTS):
        go(dn_copy(1, j))
    norm(0)
    for j in range(GU_CUTS):
        arrive(gu_copy(1, j))
    hidden((0, 2), (0, 1))
    arrive(routes_copy(1))
    go(routes_copy(3))
    arrive(routes_copy(2))

    def tokens_on(low, high):
        for i in range(low, high):
            arrive(tokens_copy(1, i))
            go(tokens_copy(3, i))

    half_t, half_g = TOKEN_CUTS // 2, GU_CUTS // 2
    tokens_on(0, half_t)
    for j in range(GU_CUTS):
        arrive(gu_copy(2, j))
        go(gu_copy(3, j))
    for j in range(TOKEN_CUTS):
        arrive(tokens_copy(2, j))

    def fourth(low, high):
        for j in range(low, high):
            arrive(gu_copy(4, j))
            go(gu_copy(6, j))
            go(gu_copy(5, j))
            span = TOKEN_CUTS - half_t
            tokens_on(half_t + span * j // GU_CUTS, half_t + span * (j + 1) // GU_CUTS)

    fourth(0, half_g)
    norm(2)
    fourth(half_g, half_g + 1)
    hidden((0, 2), (2, 3))
    for j in range(GU_CUTS):
        arrive(gu_copy(3, j))
    fourth(half_g + 1, half_g + 2)
    hidden((2, 4), (0, 1))
    fourth(half_g + 2, half_g + 3)
    hidden((2, 4), (2, 3))
    fourth(half_g + 3, GU_CUTS)
    for j in range(DOWN_CUTS):
        go(dn_copy(4, j))
    go(dn_copy(2, 0))
    go(dn_copy(2, 1))
    norm(1)
    for j in range(GU_CUTS):
        arrive(gu_copy(5, j))
    for j in range(GU_CUTS // 2):
        arrive(gu_copy(6, j))
        go(gu_copy(7, j))
    hidden((0, 6), (1, 2))
    for j in range(GU_CUTS // 2, GU_CUTS):
        arrive(gu_copy(6, j))
        go(gu_copy(7, j))
    hidden((4, 6), (0, 1))
    hidden((4, 6), (2, 3))
    down_next = lambda j: (arrive(dn_copy(4, j)), go(dn_copy(6, j)), go(dn_copy(5, j)))
    arrive(routes_copy(3))
    for j in range(TOKEN_CUTS):
        arrive(tokens_copy(3, j))
    norm(3)
    down_next(0)
    go(dn_copy(2, 2))
    hidden((0, 7), (3, 4))
    hidden((6, 7), (0, 3))
    arrive(dn_copy(2, 0))
    go(dn_copy(3, 0))
    down_next(1)
    go(dn_copy(2, 3))
    arrive(dn_copy(6, 0))
    go(dn_copy(7, 0))
    for j in range(GU_CUTS):
        arrive(gu_copy(7, j))
    hidden((7, 8), (0, 4))

    def down(block, j):
        return lax.dot_general(
            H[pl.ds(block * count, count), :], DN[pl.ds(j * d_rows, d_rows), :],
            (((1,), (1,)), ((), ())), preferred_element_type=jnp.float32,
        )

    def first_copy(j):
        return (remote(S.at[j], R.at[j], x_send.at[j], x_recv.at[j], to_z if j % 2 else to_x),)

    def second_copy(j):
        return (remote(ZS.at[j], ZR.at[j], z_send.at[j], z_recv.at[j], to_x if j % 2 else to_z),)

    def pass_on(j):
        arrive(first_copy(j))
        ZS[j] = (PZ[j] + R[j, count:].astype(jnp.float32)).astype(jnp.bfloat16)
        go(second_copy(j))
        ACC[j] = ACC[j] + R[j, :count].astype(jnp.float32)

    for j in range(DOWN_CUTS):
        if j + 2 < DOWN_CUTS:
            down_next(j + 2)
        if j + 4 < DOWN_CUTS:
            go(dn_copy(2, j + 4))
        if j + 1 < DOWN_CUTS:
            arrive(dn_copy(2, j + 1))
            go(dn_copy(3, j + 1))
            arrive(dn_copy(6, j + 1))
            go(dn_copy(7, j + 1))
        for k in (1, 3, 5, 7):
            arrive(dn_copy(k, j))
        near, kept = (1, 2) if j % 2 else (2, 1)
        S[j, count:] = down(3, j).astype(jnp.bfloat16)
        S[j, :count] = down(near, j).astype(jnp.bfloat16)
        go(first_copy(j))
        PZ[j] = down(kept, j)
        ACC[j] = down(0, j)
        if j >= LAG:
            pass_on(j - LAG)
    for j in range(DOWN_CUTS - LAG, DOWN_CUTS):
        pass_on(j)
    square = jnp.zeros((count, 1), jnp.float32)
    for j in range(DOWN_CUTS):
        arrive(second_copy(j))
        mixed = ACC[j] + ZR[j].astype(jnp.float32)
        ACC[j] = mixed
        square = square + jnp.sum(mixed * mixed, axis=1, keepdims=True)
    scale = lax.rsqrt(square / width + 1e-06)
    for j in range(DOWN_CUTS):
        cols = pl.ds(j * d_rows, d_rows)
        out[:, cols] = (ACC[j] * scale * post[:, cols]).astype(jnp.bfloat16)
    for copy in sent:
        copy.wait_send()


def fused(n_ep, tokens, pre_gain, post_gain, expert_ids, route_weight, w_gate, w_up, w_down):
    count, width = tokens.shape
    part = w_gate.shape[2]
    experts = n_ep * w_gate.shape[0]
    names = jnp.arange(experts, dtype=jnp.int32)[:, None, None]
    picks = jnp.where(expert_ids.T[None] == names, route_weight.T[None], 0.0)
    wr = jnp.sum(picks, axis=1)
    bf, f32 = jnp.bfloat16, jnp.float32
    cols = width // DOWN_CUTS
    anywhere = pl.BlockSpec(memory_space=pl.ANY)
    vmem = pl.BlockSpec(memory_space=pltpu.VMEM)
    dma = pltpu.SemaphoreType.DMA
    return pl.pallas_call(
        functools.partial(kernel, n_ep),
        out_shape=jax.ShapeDtypeStruct((count, width), bf),
        in_specs=[anywhere, vmem, vmem, anywhere, anywhere, anywhere, anywhere],
        out_specs=vmem,
        scratch_shapes=[
            pltpu.VMEM((4, count, width), bf),
            pltpu.VMEM((4 * count, width), bf),
            pltpu.VMEM((4, experts, count), f32),
            pltpu.VMEM((2, 4 * count, part), f32),
            pltpu.VMEM((8, width, 2 * part), bf),
            pltpu.VMEM((width, 8 * part), bf),
            pltpu.VMEM((4 * count, 8 * part), bf),
            pltpu.VMEM((DOWN_CUTS, 2 * count, cols), bf),
            pltpu.VMEM((DOWN_CUTS, 2 * count, cols), bf),
            pltpu.VMEM((DOWN_CUTS, count, cols), f32),
            pltpu.VMEM((DOWN_CUTS, count, cols), bf),
            pltpu.VMEM((DOWN_CUTS, count, cols), bf),
            pltpu.VMEM((DOWN_CUTS, count, cols), f32),
            dma((5,)),
            dma((4, TOKEN_CUTS)), dma((4, TOKEN_CUTS)), dma((4,)), dma((4,)),
            dma((8, GU_CUTS)), dma((8, GU_CUTS)), dma((8, DOWN_CUTS)), dma((8, DOWN_CUTS)),
            dma((DOWN_CUTS,)), dma((DOWN_CUTS,)), dma((DOWN_CUTS,)), dma((DOWN_CUTS,)),
        ],
        compiler_params=pltpu.CompilerParams(
            collective_id=0, has_side_effects=True, vmem_limit_bytes=VMEM_BYTES
        ),
    )(tokens, pre_gain[None], post_gain[None], wr, w_gate, w_up, w_down)


def whole_body(n_ep, n_tp, *args):
    lanes = args[5].shape[2]
    if n_ep // 2 == n_tp == 2 * 2 and args[5].shape[0] == 1 and lanes % 128 == 0:
        return fused(n_ep, *args)
    return body(*args)


def solution(mesh):
    in_specs = (
        P(("ep", "tp"), None),
        P(),
        P(),
        P(("ep", "tp"), None),
        P(("ep", "tp"), None),
        P("ep", None, "tp"),
        P("ep", None, "tp"),
        P("ep", None, "tp"),
    )
    out_specs = P(("ep", "tp"), None)
    step = functools.partial(whole_body, mesh.shape["ep"], mesh.shape["tp"])
    return jax.shard_map(step, mesh=mesh, in_specs=in_specs, out_specs=out_specs, check_vma=False)
```
